32 devices in a mesh: ep: 32 (over z, y, x, core), tp: 1.
Axes of the slice: x: 2, y: 2, z: 4, core: 2. Of those that a mesh axis runs over, the one named last changes fastest.
Arguments:
- tokens: bfloat16 [4096, 2048], P('ep'), may hold values from -6 to 6
- pre_gain: float32 [2048], replicated, may hold values from 0.1 to 1.9
- post_gain: float32 [2048], P('tp'), may hold values from 0.1 to 1.9
- expert_ids: int32 [4096, 2], P('ep'), may hold values from 0 to 31, all different within a row; in each aligned block of 128 rows (0 to 127, 128 to 255, ...) at most 12 rows name the same one
- route_weights: float32 [4096, 2], P('ep'), may hold values from 0.1 to 1
- w_gate: bfloat16 [32, 2048, 512], P('ep', None, 'tp'), may hold values from -0.125 to 0.125
- w_up: bfloat16 [32, 2048, 512], P('ep', None, 'tp'), may hold values from -0.125 to 0.125
- w_down: bfloat16 [32, 512, 2048], P('ep', None, 'tp'), may hold values from -0.25 to 0.25
Outputs:
- routed: bfloat16 [4096, 2048], P('ep', 'tp')
The draws below stay inside these ranges and needn't reach their ends.
Inputs may be any that keep to these rules, and one draw needn't show every extreme that they name: `expert_ids`: each row names 2 different experts. Among the rows of one index of ep (aligned blocks of 128 rows) no expert is named by more than 12 rows, a bound that some block reaches.
All inputs are finite; a program needn't handle non-finite values.
Results may differ from the reference program's by a relative error of at most 0.007.
Values may be sent and summed in bfloat16 or wider, within the bound.
A program may use at most 64 MiB of HBM per device.

```python
import math
import jax
import jax.numpy as jnp
import numpy as np
from jax import lax

D = 2048
FF = 512
TOP = 2
TOK_EP = 128
EXPERTS = 32
CAP = 12
TOKENS = 4096
N_EP = 32


def levels(own_key, shape, shards, least, high):
    def one(dim, blocks):
        draws = jax.random.uniform(jax.random.fold_in(jax.random.fold_in(own_key, 6), dim), (blocks,), jnp.float32, least / len(shards), high / len(shards))
        return jnp.repeat(jnp.exp(draws), shape[dim] // blocks).reshape((-1,) + (1,) * (len(shape) - dim - 1))

    loudness = one(*shards[0])
    for cut in shards[1:]:
        loudness = loudness * one(*cut)
    return loudness


def routed_block(rng, own, number, rows, count, top, limit, slope):
    order = jax.random.permutation(rng, count)
    heavy_load, ordinary = portions_of(count, rows * top, limit, slope, True), portions_of(count, rows * top, limit, slope, False)
    places = jnp.arange(count)

    def named(tallies, offset_by):
        used = int((tallies > 0).sum())
        fixed = max(1, used // 4)
        shifted = fixed + (places - fixed + offset_by * (used - fixed)) % max(1, count - fixed)
        return jnp.zeros((count,), jnp.int32).at[order[jnp.where(places < fixed, places, shifted)]].set(jnp.asarray(tallies, jnp.int32))

    tallies = jnp.where(number % 4 == 0, named(heavy_load, number // 4), named(ordinary, number - number // 4 - 1))
    mixed = jax.random.permutation(jax.random.fold_in(own, 3), count)
    giver, receiver = mixed[0:count // 2 * 2:2], mixed[1:count // 2 * 2:2]
    room = jnp.minimum(tallies[giver] - 1, limit - tallies[receiver]) // 2
    room = jnp.where((giver == order[0]) | (receiver == order[0]) | (tallies[receiver] == 0), 0, jnp.maximum(room, 0))
    shifted = jax.random.randint(jax.random.fold_in(own, 4), (count // 2,), 0, 1 << 20) % (room + 1)
    tallies = tallies.at[giver].add(-shifted).at[receiver].add(shifted)
    labels = jnp.searchsorted(jnp.cumsum(tallies), jnp.arange(rows * top), side="right").astype(jnp.int32)
    table = labels.reshape(top, rows).T
    table = table[jax.random.permutation(jax.random.fold_in(own, 1), rows)]
    offset_by = jax.random.randint(jax.random.fold_in(own, 2), (rows, 1), 0, top)
    return jnp.take_along_axis(table, (jnp.arange(top)[None, :] + offset_by) % top, axis=1)


def portions_of(amount, total, reach, lean, full):
    loads = [(1 << 20) // math.isqrt(standing ** lean) + 1 for standing in range(1, amount + 1)]
    largest = reach if full else min(reach, max(-(-total // amount), total * loads[0] // sum(loads)))
    least = 1 if total - largest >= amount - 1 else 0
    counts, spare = [largest] + [least] * (amount - 1), total - largest - least * (amount - 1)
    while spare > 0:
        movable = [i for i in range(1, amount) if counts[i] < largest] or [i for i in range(1, amount) if counts[i] < reach]
        mass, left = sum([loads[i] for i in movable]), spare
        for i in movable:
            more = min(reach - counts[i], max(1, left * loads[i] // mass), spare)
            counts[i] = counts[i] + more
            spare = spare - more
    return np.array(counts)


def centred(key, dims, spread, bound, cuts=(), kind=jnp.bfloat16):
    loudness = levels(key, dims, cuts, -0.22, 0.18) if cuts else 1.0
    drawn = jax.random.normal(key, dims, jnp.float32) * spread * loudness
    return jnp.minimum(jnp.maximum(drawn, -bound), bound).astype(kind)


def setup_inputs(seed: int = 0) -> dict:
    key_of = jax.random.split(jax.random.key(seed), 9)
    tokens = centred(key_of[0], (TOKENS, D), 1.0, 6.0, ((0, 32),))
    pre_gain = jnp.clip(1.0 + 0.18 * jax.random.normal(key_of[1], (D,), jnp.float32), 0.1, 1.9)
    post_gain = jnp.clip(1.0 + 0.18 * jax.random.normal(key_of[2], (D,), jnp.float32), 0.1, 1.9)
    expert_ids_keys = jax.random.split(jax.random.fold_in(key_of[3], 1), TOKENS // TOK_EP)
    expert_ids_turns = jax.random.permutation(jax.random.fold_in(key_of[3], 3), TOKENS // TOK_EP)
    expert_ids = jax.vmap(lambda own, number: routed_block(jax.random.fold_in(key_of[3], 2), own, number, TOK_EP, EXPERTS, TOP, CAP, 2))(expert_ids_keys, expert_ids_turns).reshape((TOKENS, TOP))
    route_weights = jnp.clip(0.1 + 0.9 * jax.random.uniform(key_of[4], (TOKENS, TOP), jnp.float32) ** levels(key_of[4], (TOKENS, TOP), ((0, 32),), -0.2, 0.2), 0.1, 1.0)
    w_gate = centred(key_of[5], (EXPERTS, D, FF), D ** -0.5, 0.125, ((0, 32),))
    w_up = centred(key_of[6], (EXPERTS, D, FF), D ** -0.5, 0.125, ((0, 32),))
    w_down = centred(key_of[7], (EXPERTS, FF, D), FF ** -0.5, 0.25, ((0, 32),))
    return dict(tokens=tokens, pre_gain=pre_gain, post_gain=post_gain, expert_ids=expert_ids, route_weights=route_weights, w_gate=w_gate, w_up=w_up, w_down=w_down)


epsilon = 1e-06

def reference(tokens, pre_gain, post_gain, expert_ids, route_weights, w_gate, w_up, w_down):
    total_rows, row_width = tokens.shape
    values = tokens.astype(jnp.float32)
    row_scale = lax.rsqrt(lax.optimization_barrier(jnp.mean(values * values, axis=1, keepdims=True)) + epsilon)
    normed = (values * row_scale * pre_gain[None, :]).astype(jnp.bfloat16)
    expert_count = w_gate.shape[0]
    pick_count = expert_ids.shape[1]
    block_count = N_EP
    block_rows = total_rows // block_count
    pick_total = block_rows * pick_count
    flat_ids = expert_ids.reshape(block_count, pick_total).astype(jnp.int32)
    onehot = (flat_ids[:, :, None] == jnp.arange(expert_count, dtype=jnp.int32)[None, None, :]).astype(jnp.int32)
    earlier = jnp.cumsum(onehot, axis=1) - onehot
    slot_index = lax.optimization_barrier(jnp.sum(earlier * onehot, axis=2)).astype(jnp.int32)
    block_index = jnp.broadcast_to(jnp.arange(block_count, dtype=jnp.int32)[:, None], (block_count, pick_total))
    token_index = block_index * block_rows + (jnp.arange(pick_total, dtype=jnp.int32) // pick_count)[None, :]
    owners = jnp.full((expert_count, block_count, CAP), -1, jnp.int32).at[flat_ids, block_index, slot_index].set(token_index)
    weight_of = jnp.zeros((expert_count, block_count, CAP), jnp.float32).at[flat_ids, block_index, slot_index].set(route_weights.reshape(block_count, pick_total))

    def one_expert(mixed, items):
        owner_rows, weights, gate_w, up_w, down_w = items
        owner_rows = owner_rows.reshape(-1)
        live = owner_rows >= 0
        safe_rows = jnp.where(live, owner_rows, 0)
        gathered = normed[safe_rows]
        gate_sum = jnp.dot(gathered, gate_w, preferred_element_type=jnp.float32)
        up_sum = jnp.dot(gathered, up_w, preferred_element_type=jnp.float32)
        hidden = (jax.nn.silu(gate_sum) * up_sum).astype(jnp.bfloat16)
        expert_out = jnp.dot(hidden, down_w, preferred_element_type=jnp.float32).astype(jnp.bfloat16)
        expert_out = lax.optimization_barrier(expert_out).astype(jnp.float32)
        added = jnp.where(live[:, None], expert_out * weights.reshape(-1)[:, None], 0.0)
        return (mixed.at[safe_rows].add(added), None)
    start = jnp.zeros((total_rows, row_width), jnp.float32)
    mixed, _ = lax.scan(one_expert, start, (owners, weight_of, w_gate, w_up, w_down))
    out_scale = lax.rsqrt(lax.optimization_barrier(jnp.mean(mixed * mixed, axis=1, keepdims=True)) + epsilon)
    return (mixed * out_scale * post_gain[None, :]).astype(jnp.bfloat16)
```

```python
import functools
import jax
import jax.numpy as jnp
from jax import lax
from jax.experimental import pallas as pl
from jax.experimental.pallas import tpu as pltpu
from jax.sharding import PartitionSpec as P

epsilon = 1e-06
CUTS = 4
GROUP = 4


def fused_kernel(
    n, cap, tok_ref, pre_ref, post_ref, ids_ref, rw_ref, wg_hbm, wu_hbm, wd_hbm, out_ref,
    wg, wu, wd, normed, out_buf, in_buf, res_buf, ret_buf, perm, mixed,
    wsem, send1, recv1, send2, recv2,
):
    rows, width = tok_ref.shape
    part = width // CUTS
    block = CUTS * cap
    gb = GROUP * block
    gc = GROUP * cap
    groups = n // GROUP
    side = groups // 2
    me = lax.axis_index("ep")
    tp = lax.axis_index("tp")
    mg = me // GROUP
    half = mg // side
    spot = mg % side

    weights = [
        pltpu.make_async_copy(a.at[0], b, wsem.at[i])
        for i, (a, b) in enumerate(((wg_hbm, wg), (wu_hbm, wu), (wd_hbm, wd)))
    ]
    for w in weights:
        w.start()

    barrier = pltpu.get_barrier_semaphore()

    def greet(i, c):
        peer = (me + i) % n
        pl.semaphore_signal(barrier, inc=1, device_id=(peer, tp), device_id_type=pl.DeviceIdType.MESH)
        return c

    lax.fori_loop(1, n, greet, 0)

    values = tok_ref[...].astype(jnp.float32)
    scale = lax.rsqrt(jnp.mean(values * values, axis=1, keepdims=True) + epsilon)
    normed[...] = (values * scale * pre_ref[...]).astype(jnp.bfloat16)

    lanes = max(128, n)
    expert = lax.broadcasted_iota(jnp.int32, (rows, lanes), 1)
    ids0 = ids_ref[:, 0:1]
    ids1 = ids_ref[:, 1:2]
    hot0 = (ids0 == expert).astype(jnp.float32)
    hot1 = (ids1 == expert).astype(jnp.float32)
    tri = (
        lax.broadcasted_iota(jnp.int32, (rows, rows), 1)
        < lax.broadcasted_iota(jnp.int32, (rows, rows), 0)
    ).astype(jnp.bfloat16)
    earlier = jnp.dot(tri, (hot0 + hot1).astype(jnp.bfloat16), preferred_element_type=jnp.float32)
    target0 = ids0.astype(jnp.float32) * cap + jnp.sum(earlier * hot0, axis=1, keepdims=True)
    target1 = ids1.astype(jnp.float32) * cap + jnp.sum(earlier * hot1, axis=1, keepdims=True)
    lane = lax.broadcasted_iota(jnp.int32, (rows, rows), 1)
    flipped = jnp.where(lane == 0, target0, jnp.where(lane == 1, target1, -1.0)).T
    trow0 = flipped[0:1, :].astype(jnp.int32)
    trow1 = flipped[1:2, :].astype(jnp.int32)
    tcol = jnp.concatenate([target0, target1], axis=0).astype(jnp.int32)

    u = lax.broadcasted_iota(jnp.int32, (gb, gb), 0)
    v = lax.broadcasted_iota(jnp.int32, (gb, gb), 1)
    vu = (v % block) // cap * gc + v // block * cap + v % cap
    perm[...] = (u == vu).astype(jnp.bfloat16)

    wrow = lax.broadcasted_iota(jnp.int32, (gb, rows), 0)
    wslot = wrow // block * cap + wrow % cap
    wcut = (lax.broadcasted_iota(jnp.int32, (gb, part), 0) % block) // cap

    def span(start, size):
        return pl.ds(pl.multiple_of(start, size), size)

    def give(peer):
        return pltpu.make_async_remote_copy(
            src_ref=out_buf.at[span(peer * block, block)],
            dst_ref=in_buf.at[span(me * block, block)],
            send_sem=send1.at[peer], recv_sem=recv1.at[me],
            device_id=(peer, tp), device_id_type=pl.DeviceIdType.MESH,
        )

    def take(peer):
        return pltpu.make_async_remote_copy(
            src_ref=out_buf.at[span(peer * block, block)],
            dst_ref=in_buf.at[span(peer * block, block)],
            send_sem=send1.at[peer], recv_sem=recv1.at[peer],
            device_id=(peer, tp), device_id_type=pl.DeviceIdType.MESH,
        )

    def give_back(peer):
        return pltpu.make_async_remote_copy(
            src_ref=res_buf.at[span(peer * block, block)],
            dst_ref=ret_buf.at[span(me * block, block)],
            send_sem=send2.at[peer], recv_sem=recv2.at[me],
            device_id=(peer, tp), device_id_type=pl.DeviceIdType.MESH,
        )

    def take_back(peer):
        return pltpu.make_async_remote_copy(
            src_ref=res_buf.at[span(peer * block, block)],
            dst_ref=ret_buf.at[span(peer * block, block)],
            send_sem=send2.at[peer], recv_sem=recv2.at[peer],
            device_id=(peer, tp), device_id_type=pl.DeviceIdType.MESH,
        )

    def each(g, do):
        def one(j, c):
            peer = g * GROUP + (me + j) % GROUP

            @pl.when(peer != me)
            def _():
                do(peer)

            return c

        lax.fori_loop(0, GROUP, one, 0)

    def far(i, sign):
        return (1 - half) * side + (spot + side + sign * i) % side

    def near(i, sign):
        return half * side + (spot + side + sign * i) % side

    def dispatch(g):
        want = wslot + g * gc
        pick = ((trow0 == want) | (trow1 == want)).astype(jnp.bfloat16)
        spread = jnp.dot(pick, normed[...], preferred_element_type=jnp.float32)
        chosen = spread[:, 0:part]
        for q in range(1, CUTS):
            chosen = jnp.where(wcut == q, spread[:, q * part:(q + 1) * part], chosen)
        out_buf[span(g * gb, gb), :] = chosen.astype(jnp.bfloat16)

    pl.semaphore_wait(barrier, n - 1)

    def send_step(i, c):
        for which in (far, near):
            g = which(i, 1)
            dispatch(g)
            each(g, lambda peer: give(peer).start())
        return c

    lax.fori_loop(0, side, send_step, 0)
    mine = span(me * block, block)
    in_buf[mine, :] = out_buf[mine, :]
    for w in weights:
        w.wait()

    def experts(g):
        each(g, lambda peer: take(peer).wait_recv())
        here = span(g * gb, gb)
        stacked = jnp.dot(perm[...], in_buf[here, :], preferred_element_type=jnp.float32).astype(jnp.bfloat16)
        x = jnp.concatenate([stacked[q * gc:(q + 1) * gc, :] for q in range(CUTS)], axis=1)
        gate = jnp.dot(x, wg[...], preferred_element_type=jnp.float32)
        up = jnp.dot(x, wu[...], preferred_element_type=jnp.float32)
        hidden = (gate / (1.0 + jnp.exp(-gate)) * up).astype(jnp.bfloat16)
        y = jnp.dot(hidden, wd[...], preferred_element_type=jnp.float32).astype(jnp.bfloat16)
        back = jnp.concatenate([y[:, q * part:(q + 1) * part] for q in range(CUTS)], axis=0)
        wire = lax.dot_general(perm[...], back, (((0,), (0,)), ((), ())), preferred_element_type=jnp.float32)
        res_buf[here, :] = wire.astype(jnp.bfloat16)
        each(g, lambda peer: give_back(peer).start())

    def expert_step(i, c):
        experts(near(i, -1))
        experts(far(i, -1))
        return c

    lax.fori_loop(0, side, expert_step, 0)
    ret_buf[mine, :] = res_buf[mine, :]

    w0 = rw_ref[:, 0:1]
    w1 = rw_ref[:, 1:2]
    mixed[...] = jnp.zeros_like(mixed)
    pcol = lax.broadcasted_iota(jnp.int32, (2 * rows, gc), 1)

    def combine(g):
        each(g, lambda peer: take_back(peer).wait_recv())
        stacked = jnp.dot(
            perm[...], ret_buf[span(g * gb, gb), :], preferred_element_type=jnp.float32
        ).astype(jnp.bfloat16)
        z = jnp.concatenate([stacked[q * gc:(q + 1) * gc, :] for q in range(CUTS)], axis=1)
        pick = (tcol == pcol + g * gc).astype(jnp.bfloat16)
        got = jnp.dot(pick, z, preferred_element_type=jnp.float32)
        mixed[...] += got[:rows] * w0 + got[rows:] * w1

    def near_step(i, c):
        combine(near(i, 1))
        return c

    def far_step(i, c):
        combine(far(i, 1))
        return c

    lax.fori_loop(0, side, near_step, 0)
    lax.fori_loop(0, side, far_step, 0)

    total = mixed[...]
    out_scale = lax.rsqrt(jnp.mean(total * total, axis=1, keepdims=True) + epsilon)
    out_ref[...] = (total * out_scale * post_ref[...]).astype(jnp.bfloat16)

    def drain(i, c):
        peer = (me + i) % n
        give(peer).wait_send()
        give_back(peer).wait_send()
        return c

    lax.fori_loop(1, n, drain, 0)


def fused(n, cap, tokens, pre_gain, post_gain, expert_ids, route_weights, w_gate, w_up, w_down):
    rows, width = tokens.shape
    hidden = w_gate.shape[2]
    part = width // CUTS
    block = CUTS * cap
    gb = GROUP * block
    vmem = pl.BlockSpec(memory_space=pltpu.VMEM)
    hbm = pl.BlockSpec(memory_space=pl.ANY)
    buf = pltpu.VMEM((n * block, part), jnp.bfloat16)
    return pl.pallas_call(
        functools.partial(fused_kernel, n, cap),
        out_shape=jax.ShapeDtypeStruct((rows, width), jnp.bfloat16),
        in_specs=[vmem] * 5 + [hbm] * 3,
        out_specs=vmem,
        scratch_shapes=[
            pltpu.VMEM((width, hidden), jnp.bfloat16),
            pltpu.VMEM((width, hidden), jnp.bfloat16),
            pltpu.VMEM((hidden, width), jnp.bfloat16),
            pltpu.VMEM((rows, width), jnp.bfloat16),
            buf, buf, buf, buf,
            pltpu.VMEM((gb, gb), jnp.bfloat16),
            pltpu.VMEM((rows, width), jnp.float32),
            pltpu.SemaphoreType.DMA((3,)),
            pltpu.SemaphoreType.DMA((n,)),
            pltpu.SemaphoreType.DMA((n,)),
            pltpu.SemaphoreType.DMA((n,)),
            pltpu.SemaphoreType.DMA((n,)),
        ],
        compiler_params=pltpu.CompilerParams(collective_id=0, has_side_effects=True),
    )(
        tokens, pre_gain.reshape(1, width), post_gain.reshape(1, width), expert_ids, route_weights,
        w_gate, w_up, w_down,
    )


def per_device(tokens, pre_gain, post_gain, expert_ids, route_weights, w_gate, w_up, w_down):
    tok_rows, row_width = tokens.shape
    pick_count = expert_ids.shape[1]
    ep_count = lax.axis_size("ep")
    local_experts = w_gate.shape[0]
    experts = ep_count * local_experts
    capacity = 3 * tok_rows * pick_count // (2 * experts)
    pick_total = tok_rows * pick_count
    flat_ids = expert_ids.reshape(pick_total)
    onehot = (flat_ids[:, None] == jnp.arange(experts, dtype=jnp.int32)[None, :]).astype(
        jnp.bfloat16
    )
    positions = jnp.arange(pick_total, dtype=jnp.int32)
    strict_lower = (positions[None, :] < positions[:, None]).astype(jnp.bfloat16)
    earlier = jnp.dot(strict_lower, onehot, preferred_element_type=jnp.float32)
    slot_index = jnp.sum(earlier * onehot, axis=1).astype(jnp.int32)
    target = flat_ids * capacity + slot_index
    values = tokens.astype(jnp.float32)
    row_scale = lax.rsqrt(jnp.mean(values * values, axis=1, keepdims=True) + epsilon)
    normed = (values * row_scale * pre_gain[None, :]).astype(jnp.bfloat16)
    sent_width = normed.shape[1]
    copies = jnp.broadcast_to(normed[:, None, :], (tok_rows, pick_count, sent_width)).reshape(
        pick_total, sent_width
    )
    buffer = jnp.zeros((experts * capacity, sent_width), jnp.bfloat16).at[target].set(copies)
    arrived = lax.all_to_all(buffer, "ep", split_axis=0, concat_axis=0, tiled=True)
    rows_in = arrived.reshape(ep_count, local_experts, capacity, row_width)
    gate_sum = jnp.einsum("sxcd,xdf->sxcf", rows_in, w_gate, preferred_element_type=jnp.float32)
    up_sum = jnp.einsum("sxcd,xdf->sxcf", rows_in, w_up, preferred_element_type=jnp.float32)
    hidden = (jax.nn.silu(gate_sum) * up_sum).astype(jnp.bfloat16)
    out_cols = w_down.shape[2]
    produced = jnp.einsum(
        "sxcf,xfd->sxcd",
        lax.all_gather(hidden, "tp", axis=3, tiled=True),
        w_down,
        preferred_element_type=jnp.float32,
    )
    results = produced.astype(jnp.bfloat16).reshape(experts * capacity, out_cols)
    returned = lax.all_to_all(results, "ep", split_axis=0, concat_axis=0, tiled=True)
    picked = returned[target].astype(jnp.float32) * route_weights.reshape(pick_total)[:, None]
    mixed = jnp.sum(picked.reshape(tok_rows, pick_count, out_cols), axis=1)
    squares = lax.psum(jnp.sum(mixed * mixed, axis=1), "tp")
    out_scale = lax.rsqrt(squares / row_width + epsilon)
    return (mixed * out_scale[:, None] * post_gain[None, :]).astype(jnp.bfloat16)


def per_shard(n, tp, tokens, *rest):
    pre_gain, post_gain, expert_ids, route_weights, w_gate, w_up, w_down = rest
    rows, width = tokens.shape
    picks = expert_ids.shape[1]
    cap = 3 * rows * picks // (2 * n * w_gate.shape[0])
    fits = (
        tp == 1 and picks == 2 and w_gate.shape[0] == 1 and n % (2 * GROUP) == 0 and n <= 128
        and rows == 128 and (CUTS * cap) % 16 == 0 and cap > 0 and width % (CUTS * 128) == 0
    )
    if fits:
        return fused(n, cap, tokens, *rest)
    return per_device(tokens, *rest)


def solution(mesh):
    placed = (
        P("ep", None),
        P(),
        P("tp"),
        P("ep", None),
        P("ep", None),
        P("ep", None, "tp"),
        P("ep", None, "tp"),
        P("ep", None, "tp"),
    )
    return jax.shard_map(
        functools.partial(per_shard, mesh.shape["ep"], mesh.shape["tp"]),
        mesh=mesh, in_specs=placed, out_specs=P("ep", "tp"), check_vma=False,
    )
```

```python
import functools
import jax
import jax.numpy as jnp
from jax import lax
from jax.experimental import pallas as pl
from jax.experimental.pallas import tpu as pltpu
from jax.sharding import PartitionSpec as P

epsilon = 1e-06
CUTS = 4
GROUP = 4
EARLY = 2


def fused_kernel(
    n, cap, tok_ref, pre_ref, post_ref, ids_ref, rw_ref, wg_hbm, wu_hbm, wd_hbm, out_ref,
    wg, wu, wd, toks, meta, part_out, part_in, out_buf, in_buf, res_buf, ret_buf, perm, mixed,
    wsem, send1, recv1, send2, recv2, xsend, xrecv,
):
    rows, width = tok_ref.shape
    part = width // CUTS
    block = CUTS * cap
    gb = GROUP * block
    gc = GROUP * cap
    groups = n // GROUP
    side = groups // 2
    quarter = n // 4
    gq = groups // 4
    me = lax.axis_index("ep")
    tp = lax.axis_index("tp")
    mg = me // GROUP
    half = mg // side
    spot = mg % side
    plane = me // quarter
    is_mid = (plane == 1) | (plane == 2)
    partner = jnp.where(plane == 1, me + quarter, jnp.where(plane == 2, me - quarter, me))
    guest = jnp.where(is_mid, 1, 0)
    other = (me + n // 2) % n
    MESH = pl.DeviceIdType.MESH

    weights = [
        pltpu.make_async_copy(a.at[0], b, wsem.at[i])
        for i, (a, b) in enumerate(((wg_hbm, wg), (wu_hbm, wu), (wd_hbm, wd)))
    ]
    for w in weights:
        w.start()

    barrier = pltpu.get_barrier_semaphore()

    def greet(i, c):
        pl.semaphore_signal(barrier, inc=1, device_id=((me + i) % n, tp), device_id_type=MESH)
        return c

    lax.fori_loop(1, n, greet, 0)

    values = tok_ref[...].astype(jnp.float32)
    scale = lax.rsqrt(jnp.mean(values * values, axis=1, keepdims=True) + epsilon)
    toks[0:rows, :] = (values * scale * pre_ref[...]).astype(jnp.bfloat16)

    sub = lax.broadcasted_iota(jnp.int32, (rows, rows), 0)
    lane = lax.broadcasted_iota(jnp.int32, (rows, rows), 1)

    def columns(four):
        spread = jnp.where(sub == 3, four[3], 0.0)
        for i in range(3):
            spread = jnp.where(sub == i, four[i], spread)
        turned = spread.T
        return [turned[:, i:i + 1] for i in range(4)]

    w0row, w1row = rw_ref[0:1, :], rw_ref[1:2, :]
    ids0, ids1, _, _ = columns(
        [ids_ref[0:1, :].astype(jnp.float32), ids_ref[1:2, :].astype(jnp.float32), w0row, w1row]
    )
    expert = lane.astype(jnp.float32)
    hot0 = (ids0 == expert).astype(jnp.float32)
    hot1 = (ids1 == expert).astype(jnp.float32)
    tri = (lane < sub).astype(jnp.bfloat16)
    earlier = jnp.dot(tri, (hot0 + hot1).astype(jnp.bfloat16), preferred_element_type=jnp.float32)
    target0 = ids0 * cap + jnp.sum(earlier * hot0, axis=1, keepdims=True)
    target1 = ids1 * cap + jnp.sum(earlier * hot1, axis=1, keepdims=True)
    flipped = jnp.where(lane == 0, target0, jnp.where(lane == 1, target1, -1.0)).T
    eight = lax.broadcasted_iota(jnp.int32, (8, rows), 0)
    table = jnp.where(eight == 0, flipped[0:1, :], jnp.where(eight == 1, flipped[1:2, :], 0.0))
    meta[0:8, :] = jnp.where(eight == 2, w0row, jnp.where(eight == 3, w1row, table))

    def span(start, size):
        return pl.ds(pl.multiple_of(start, size), size)

    def swap(i, src, dst):
        return pltpu.make_async_remote_copy(
            src_ref=src, dst_ref=dst, send_sem=xsend.at[i], recv_sem=xrecv.at[i],
            device_id=(partner, tp), device_id_type=MESH,
        )

    swaps = [
        swap(0, meta.at[pl.ds(0, 8)], meta.at[pl.ds(8, 8)]),
        swap(1, toks.at[pl.ds(0, rows)], toks.at[pl.ds(rows, rows)]),
        swap(2, part_out, part_in),
    ]

    pl.semaphore_wait(barrier, n - 1)

    @pl.when(is_mid)
    def _():
        swaps[0].start()
        swaps[1].start()

    u = lax.broadcasted_iota(jnp.int32, (gb, gb), 0)
    v = lax.broadcasted_iota(jnp.int32, (gb, gb), 1)
    vu = (v % block) // cap * gc + v // block * cap + v % cap
    perm[...] = (u == vu).astype(jnp.bfloat16)

    wrow = lax.broadcasted_iota(jnp.int32, (gb, rows), 0)
    wslot = wrow // block * cap + wrow % cap
    wcut = (lax.broadcasted_iota(jnp.int32, (gb, part), 0) % block) // cap

    def relayed(slot):
        return is_mid & (slot // (n // 2) != half)

    def target_of(slot):
        return jnp.where(relayed(slot), (slot + n // 2) % n, slot)

    def guested(s):
        q = s // quarter
        return ((q == 1) | (q == 2)) & (s // (n // 2) != half)

    def carrier(s):
        q = s // quarter
        return jnp.where(guested(s), jnp.where(q == 1, s + quarter, s - quarter), s)

    def give(slot):
        source = jnp.where(relayed(slot), partner, me)
        return pltpu.make_async_remote_copy(
            src_ref=out_buf.at[span(slot * block, block)],
            dst_ref=in_buf.at[span(source * block, block)],
            send_sem=send1.at[slot], recv_sem=recv1.at[source],
            device_id=(target_of(slot), tp), device_id_type=MESH,
        )

    def take(s):
        return pltpu.make_async_remote_copy(
            src_ref=out_buf.at[span(s * block, block)],
            dst_ref=in_buf.at[span(s * block, block)],
            send_sem=send1.at[s], recv_sem=recv1.at[s],
            device_id=(carrier(s), tp), device_id_type=MESH,
        )

    def give_back(s):
        slot = jnp.where(guested(s), other, me)
        return pltpu.make_async_remote_copy(
            src_ref=res_buf.at[span(s * block, block)],
            dst_ref=ret_buf.at[span(slot * block, block)],
            send_sem=send2.at[s], recv_sem=recv2.at[slot],
            device_id=(carrier(s), tp), device_id_type=MESH,
        )

    def take_back(slot):
        return pltpu.make_async_remote_copy(
            src_ref=res_buf.at[span(slot * block, block)],
            dst_ref=ret_buf.at[span(slot * block, block)],
            send_sem=send2.at[slot], recv_sem=recv2.at[slot],
            device_id=(target_of(slot), tp), device_id_type=MESH,
        )

    def each(g, device, do):
        def one(j, c):
            index = g * GROUP + (me + j) % GROUP

            @pl.when(device(index) != me)
            def _():
                do(index)

            return c

        lax.fori_loop(0, GROUP, one, 0)

    def far(i, sign):
        return (1 - half) * side + (spot + side + sign * i) % side

    def near(i, sign):
        return half * side + (spot + side + sign * i) % side

    def dispatch(g, which, real):
        lines = meta[span(which * 8, 8), :]
        want = (wslot + real * gc).astype(jnp.float32)
        pick = ((lines[0:1, :] == want) | (lines[1:2, :] == want)).astype(jnp.bfloat16)
        spread = jnp.dot(pick, toks[span(which * rows, rows), :], preferred_element_type=jnp.float32)
        chosen = spread[:, 0:part]
        for q in range(1, CUTS):
            chosen = jnp.where(wcut == q, spread[:, q * part:(q + 1) * part], chosen)
        out_buf[span(g * gb, gb), :] = chosen.astype(jnp.bfloat16)
        each(g, target_of, lambda slot: give(slot).start())

    def real_group(g):
        return jnp.where(is_mid, (g + side) % groups, g)

    def near_send(i, c):
        g = near(i, 1)
        dispatch(g, 0, g)
        return c

    def far_send(i, c):
        g = far(i, 1)
        dispatch(g, guest, real_group(g))
        return c

    mine = span(me * block, block)
    theirs = span(partner * block, block)
    across = span(other * block, block)

    lax.fori_loop(0, side, near_send, 0)
    in_buf[mine, :] = out_buf[mine, :]

    @pl.when(jnp.logical_not(is_mid))
    def _():
        lax.fori_loop(0, side, far_send, 0)

    for w in weights:
        w.wait()

    def experts(g):
        each(g, carrier, lambda s: take(s).wait_recv())
        here = span(g * gb, gb)
        stacked = jnp.dot(perm[...], in_buf[here, :], preferred_element_type=jnp.float32).astype(jnp.bfloat16)
        x = jnp.concatenate([stacked[q * gc:(q + 1) * gc, :] for q in range(CUTS)], axis=1)
        gate = jnp.dot(x, wg[...], preferred_element_type=jnp.float32)
        up = jnp.dot(x, wu[...], preferred_element_type=jnp.float32)
        hidden = (gate / (1.0 + jnp.exp(-gate)) * up).astype(jnp.bfloat16)
        y = jnp.dot(hidden, wd[...], preferred_element_type=jnp.float32).astype(jnp.bfloat16)
        back = jnp.concatenate([y[:, q * part:(q + 1) * part] for q in range(CUTS)], axis=0)
        wire = lax.dot_general(perm[...], back, (((0,), (0,)), ((), ())), preferred_element_type=jnp.float32)
        res_buf[here, :] = wire.astype(jnp.bfloat16)
        each(g, carrier, lambda s: give_back(s).start())

    def near_experts(i, c):
        experts(near(i, -1))
        return c

    def far_experts(i, c):
        q = jnp.where(i < gq, 2 - half, 3 * (1 - half))
        experts(q * gq + (mg + gq - i % gq) % gq)
        return c

    lax.fori_loop(0, EARLY, near_experts, 0)

    @pl.when(is_mid)
    def _():
        swaps[0].wait_recv()
        swaps[1].wait_recv()
        lax.fori_loop(0, side, far_send, 0)
        in_buf[theirs, :] = out_buf[across, :]

    lax.fori_loop(EARLY, side, near_experts, 0)
    lax.fori_loop(0, side, far_experts, 0)
    ret_buf[mine, :] = res_buf[mine, :]

    pcol = lax.broadcasted_iota(jnp.int32, (rows, gc), 1)

    def combine(first, which, shift):
        lines = meta[span(which * 8, 8), :]
        t0, t1, w0, w1 = columns([lines[i:i + 1, :] for i in range(4)])

        def step(i, c):
            g = first(i, 1)
            each(g, target_of, lambda slot: take_back(slot).wait_recv())
            stacked = jnp.dot(
                perm[...], ret_buf[span(g * gb, gb), :], preferred_element_type=jnp.float32
            ).astype(jnp.bfloat16)
            z = jnp.concatenate([stacked[q * gc:(q + 1) * gc, :] for q in range(CUTS)], axis=1)
            want = (pcol + shift(g) * gc).astype(jnp.float32)
            got0 = jnp.dot((t0 == want).astype(jnp.bfloat16), z, preferred_element_type=jnp.float32)
            got1 = jnp.dot((t1 == want).astype(jnp.bfloat16), z, preferred_element_type=jnp.float32)
            mixed[...] += got0 * w0 + got1 * w1
            return c

        lax.fori_loop(0, side, step, 0)

    mixed[...] = jnp.zeros_like(mixed)

    @pl.when(is_mid)
    def _():
        ret_buf[across, :] = res_buf[theirs, :]
        combine(far, guest, real_group)
        part_out[...] = mixed[...].astype(jnp.bfloat16)
        swaps[2].start()
        mixed[...] = jnp.zeros_like(mixed)

    combine(near, 0, lambda g: g)

    @pl.when(jnp.logical_not(is_mid))
    def _():
        combine(far, guest, real_group)

    @pl.when(is_mid)
    def _():
        swaps[2].wait_recv()
        mixed[...] += part_in[...].astype(jnp.float32)

    total = mixed[...]
    out_scale = lax.rsqrt(jnp.mean(total * total, axis=1, keepdims=True) + epsilon)
    out_ref[...] = (total * out_scale * post_ref[...]).astype(jnp.bfloat16)

    def drain(i, c):
        @pl.when(target_of(i) != me)
        def _():
            give(i).wait_send()

        @pl.when(carrier(i) != me)
        def _():
            give_back(i).wait_send()

        return c

    lax.fori_loop(0, n, drain, 0)

    @pl.when(is_mid)
    def _():
        for s in swaps:
            s.wait_send()


def fused(n, cap, tokens, pre_gain, post_gain, expert_ids, route_weights, w_gate, w_up, w_down):
    rows, width = tokens.shape
    hidden = w_gate.shape[2]
    part = width // CUTS
    block = CUTS * cap
    gb = GROUP * block
    vmem = pl.BlockSpec(memory_space=pltpu.VMEM)
    hbm = pl.BlockSpec(memory_space=pl.ANY)
    buf = pltpu.VMEM((n * block, part), jnp.bfloat16)
    return pl.pallas_call(
        functools.partial(fused_kernel, n, cap),
        out_shape=jax.ShapeDtypeStruct((rows, width), jnp.bfloat16),
        in_specs=[vmem] * 5 + [hbm] * 3,
        out_specs=vmem,
        scratch_shapes=[
            pltpu.VMEM((width, hidden), jnp.bfloat16),
            pltpu.VMEM((width, hidden), jnp.bfloat16),
            pltpu.VMEM((hidden, width), jnp.bfloat16),
            pltpu.VMEM((2 * rows, width), jnp.bfloat16),
            pltpu.VMEM((16, rows), jnp.float32),
            pltpu.VMEM((rows, width), jnp.bfloat16),
            pltpu.VMEM((rows, width), jnp.bfloat16),
            buf, buf, buf, buf,
            pltpu.VMEM((gb, gb), jnp.bfloat16),
            pltpu.VMEM((rows, width), jnp.float32),
            pltpu.SemaphoreType.DMA((3,)),
            pltpu.SemaphoreType.DMA((n,)),
            pltpu.SemaphoreType.DMA((n,)),
            pltpu.SemaphoreType.DMA((n,)),
            pltpu.SemaphoreType.DMA((n,)),
            pltpu.SemaphoreType.DMA((3,)),
            pltpu.SemaphoreType.DMA((3,)),
        ],
        compiler_params=pltpu.CompilerParams(collective_id=0, has_side_effects=True),
    )(
        tokens, pre_gain.reshape(1, width), post_gain.reshape(1, width), expert_ids.T, route_weights.T,
        w_gate, w_up, w_down,
    )


def per_device(tokens, pre_gain, post_gain, expert_ids, route_weights, w_gate, w_up, w_down):
    tok_rows, row_width = tokens.shape
    pick_count = expert_ids.shape[1]
    ep_count = lax.axis_size("ep")
    local_experts = w_gate.shape[0]
    experts = ep_count * local_experts
    capacity = 3 * tok_rows * pick_count // (2 * experts)
    pick_total = tok_rows * pick_count
    flat_ids = expert_ids.reshape(pick_total)
    onehot = (flat_ids[:, None] == jnp.arange(experts, dtype=jnp.int32)[None, :]).astype(
        jnp.bfloat16
    )
    positions = jnp.arange(pick_total, dtype=jnp.int32)
    strict_lower = (positions[None, :] < positions[:, None]).astype(jnp.bfloat16)
    earlier = jnp.dot(strict_lower, onehot, preferred_element_type=jnp.float32)
    slot_index = jnp.sum(earlier * onehot, axis=1).astype(jnp.int32)
    target = flat_ids * capacity + slot_index
    values = tokens.astype(jnp.float32)
    row_scale = lax.rsqrt(jnp.mean(values * values, axis=1, keepdims=True) + epsilon)
    normed = (values * row_scale * pre_gain[None, :]).astype(jnp.bfloat16)
    sent_width = normed.shape[1]
    copies = jnp.broadcast_to(normed[:, None, :], (tok_rows, pick_count, sent_width)).reshape(
        pick_total, sent_width
    )
    buffer = jnp.zeros((experts * capacity, sent_width), jnp.bfloat16).at[target].set(copies)
    arrived = lax.all_to_all(buffer, "ep", split_axis=0, concat_axis=0, tiled=True)
    rows_in = arrived.reshape(ep_count, local_experts, capacity, row_width)
    gate_sum = jnp.einsum("sxcd,xdf->sxcf", rows_in, w_gate, preferred_element_type=jnp.float32)
    up_sum = jnp.einsum("sxcd,xdf->sxcf", rows_in, w_up, preferred_element_type=jnp.float32)
    hidden = (jax.nn.silu(gate_sum) * up_sum).astype(jnp.bfloat16)
    out_cols = w_down.shape[2]
    produced = jnp.einsum(
        "sxcf,xfd->sxcd",
        lax.all_gather(hidden, "tp", axis=3, tiled=True),
        w_down,
        preferred_element_type=jnp.float32,
    )
    results = produced.astype(jnp.bfloat16).reshape(experts * capacity, out_cols)
    returned = lax.all_to_all(results, "ep", split_axis=0, concat_axis=0, tiled=True)
    picked = returned[target].astype(jnp.float32) * route_weights.reshape(pick_total)[:, None]
    mixed = jnp.sum(picked.reshape(tok_rows, pick_count, out_cols), axis=1)
    squares = lax.psum(jnp.sum(mixed * mixed, axis=1), "tp")
    out_scale = lax.rsqrt(squares / row_width + epsilon)
    return (mixed * out_scale[:, None] * post_gain[None, :]).astype(jnp.bfloat16)


def per_shard(n, tp, tokens, *rest):
    pre_gain, post_gain, expert_ids, route_weights, w_gate, w_up, w_down = rest
    rows, width = tokens.shape
    picks = expert_ids.shape[1]
    cap = 3 * rows * picks // (2 * n * w_gate.shape[0])
    fits = (
        tp == 1 and picks == 2 and w_gate.shape[0] == 1 and n % (4 * GROUP) == 0 and n <= 128
        and rows == 128 and (CUTS * cap) % 16 == 0 and cap > 0 and width % (CUTS * 128) == 0
    )
    if fits:
        return fused(n, cap, tokens, *rest)
    return per_device(tokens, *rest)


def solution(mesh):
    placed = (
        P("ep", None),
        P(),
        P("tp"),
        P("ep", None),
        P("ep", None),
        P("ep", None, "tp"),
        P("ep", None, "tp"),
        P("ep", None, "tp"),
    )
    return jax.shard_map(
        functools.partial(per_shard, mesh.shape["ep"], mesh.shape["tp"]),
        mesh=mesh, in_specs=placed, out_specs=P("ep", "tp"), check_vma=False,
    )
```

```python
import functools
import jax
import jax.numpy as jnp
from jax import lax
from jax.experimental import pallas as pl
from jax.experimental.pallas import tpu as pltpu
from jax.sharding import PartitionSpec as P

epsilon = 1e-06
CUTS = 4
GROUP = 4
EARLY = 2
HELD = 3
PROMPT = 0
DEFER = 3


def fused_kernel(
    n, cap, tok_ref, pre_ref, post_ref, ids_ref, rw_ref, wg_hbm, wu_hbm, wd_hbm, out_ref,
    wg, wu, wd, toks, meta, part_out, part_in, out_buf, in_buf, res_buf, ret_buf, perm, mixed,
    wsem, send1, recv1, send2, recv2, xsend, xrecv,
):
    rows, width = tok_ref.shape
    part = width // CUTS
    block = CUTS * cap
    gb = GROUP * block
    gc = GROUP * cap
    groups = n // GROUP
    side = groups // 2
    quarter = n // 4
    gq = groups // 4
    me = lax.axis_index("ep")
    tp = lax.axis_index("tp")
    mg = me // GROUP
    half = mg // side
    spot = mg % side
    plane = me // quarter
    is_mid = (plane == 1) | (plane == 2)
    partner = jnp.where(plane == 1, me + quarter, jnp.where(plane == 2, me - quarter, me))
    guest = jnp.where(is_mid, 1, 0)
    other = (me + n // 2) % n
    MESH = pl.DeviceIdType.MESH

    weights = [
        pltpu.make_async_copy(a.at[0], b, wsem.at[i])
        for i, (a, b) in enumerate(((wg_hbm, wg), (wu_hbm, wu), (wd_hbm, wd)))
    ]
    for w in weights:
        w.start()

    barrier = pltpu.get_barrier_semaphore()

    def greet(i, c):
        pl.semaphore_signal(barrier, inc=1, device_id=((me + i) % n, tp), device_id_type=MESH)
        return c

    lax.fori_loop(1, n, greet, 0)

    values = tok_ref[...].astype(jnp.float32)
    scale = lax.rsqrt(jnp.mean(values * values, axis=1, keepdims=True) + epsilon)
    toks[0:rows, :] = (values * scale * pre_ref[...]).astype(jnp.bfloat16)

    sub = lax.broadcasted_iota(jnp.int32, (rows, rows), 0)
    lane = lax.broadcasted_iota(jnp.int32, (rows, rows), 1)

    def columns(four):
        spread = jnp.where(sub == 3, four[3], 0.0)
        for i in range(3):
            spread = jnp.where(sub == i, four[i], spread)
        turned = spread.T
        return [turned[:, i:i + 1] for i in range(4)]

    w0row, w1row = rw_ref[0:1, :], rw_ref[1:2, :]
    ids0, ids1, _, _ = columns(
        [ids_ref[0:1, :].astype(jnp.float32), ids_ref[1:2, :].astype(jnp.float32), w0row, w1row]
    )
    expert = lane.astype(jnp.float32)
    hot0 = (ids0 == expert).astype(jnp.float32)
    hot1 = (ids1 == expert).astype(jnp.float32)
    tri = (lane < sub).astype(jnp.bfloat16)
    earlier = jnp.dot(tri, (hot0 + hot1).astype(jnp.bfloat16), preferred_element_type=jnp.float32)
    target0 = ids0 * cap + jnp.sum(earlier * hot0, axis=1, keepdims=True)
    target1 = ids1 * cap + jnp.sum(earlier * hot1, axis=1, keepdims=True)
    flipped = jnp.where(lane == 0, target0, jnp.where(lane == 1, target1, -1.0)).T
    eight = lax.broadcasted_iota(jnp.int32, (8, rows), 0)
    table = jnp.where(eight == 0, flipped[0:1, :], jnp.where(eight == 1, flipped[1:2, :], 0.0))
    meta[0:8, :] = jnp.where(eight == 2, w0row, jnp.where(eight == 3, w1row, table))

    def span(start, size):
        return pl.ds(pl.multiple_of(start, size), size)

    def swap(i, src, dst):
        return pltpu.make_async_remote_copy(
            src_ref=src, dst_ref=dst, send_sem=xsend.at[i], recv_sem=xrecv.at[i],
            device_id=(partner, tp), device_id_type=MESH,
        )

    swaps = [
        swap(0, meta.at[pl.ds(0, 8)], meta.at[pl.ds(8, 8)]),
        swap(1, toks.at[pl.ds(0, rows)], toks.at[pl.ds(rows, rows)]),
        swap(2, part_out, part_in),
    ]

    pl.semaphore_wait(barrier, n - 1)

    @pl.when(is_mid)
    def _():
        swaps[0].start()
        swaps[1].start()

    u = lax.broadcasted_iota(jnp.int32, (gb, gb), 0)
    v = lax.broadcasted_iota(jnp.int32, (gb, gb), 1)
    vu = (v % block) // cap * gc + v // block * cap + v % cap
    perm[...] = (u == vu).astype(jnp.bfloat16)

    wrow = lax.broadcasted_iota(jnp.int32, (gb, rows), 0)
    wslot = wrow // block * cap + wrow % cap
    wcut = (lax.broadcasted_iota(jnp.int32, (gb, part), 0) % block) // cap

    def relayed(slot):
        return is_mid & (slot // (n // 2) != half)

    def target_of(slot):
        return jnp.where(relayed(slot), (slot + n // 2) % n, slot)

    def guested(s):
        q = s // quarter
        return ((q == 1) | (q == 2)) & (s // (n // 2) != half)

    def carrier(s):
        q = s // quarter
        return jnp.where(guested(s), jnp.where(q == 1, s + quarter, s - quarter), s)

    def give(slot):
        source = jnp.where(relayed(slot), partner, me)
        return pltpu.make_async_remote_copy(
            src_ref=out_buf.at[span(slot * block, block)],
            dst_ref=in_buf.at[span(source * block, block)],
            send_sem=send1.at[slot], recv_sem=recv1.at[source],
            device_id=(target_of(slot), tp), device_id_type=MESH,
        )

    def take(s):
        return pltpu.make_async_remote_copy(
            src_ref=out_buf.at[span(s * block, block)],
            dst_ref=in_buf.at[span(s * block, block)],
            send_sem=send1.at[s], recv_sem=recv1.at[s],
            device_id=(carrier(s), tp), device_id_type=MESH,
        )

    def give_back(s):
        slot = jnp.where(guested(s), other, me)
        return pltpu.make_async_remote_copy(
            src_ref=res_buf.at[span(s * block, block)],
            dst_ref=ret_buf.at[span(slot * block, block)],
            send_sem=send2.at[s], recv_sem=recv2.at[slot],
            device_id=(carrier(s), tp), device_id_type=MESH,
        )

    def take_back(slot):
        return pltpu.make_async_remote_copy(
            src_ref=res_buf.at[span(slot * block, block)],
            dst_ref=ret_buf.at[span(slot * block, block)],
            send_sem=send2.at[slot], recv_sem=recv2.at[slot],
            device_id=(target_of(slot), tp), device_id_type=MESH,
        )

    def each(g, device, do):
        def one(j, c):
            index = g * GROUP + (me + j) % GROUP

            @pl.when(device(index) != me)
            def _():
                do(index)

            return c

        lax.fori_loop(0, GROUP, one, 0)

    def far(i, sign):
        return (1 - half) * side + (spot + side + sign * i) % side

    def near(i, sign):
        return half * side + (spot + side + sign * i) % side

    def dispatch(g, which, real):
        lines = meta[span(which * 8, 8), :]
        want = (wslot + real * gc).astype(jnp.float32)
        pick = ((lines[0:1, :] == want) | (lines[1:2, :] == want)).astype(jnp.bfloat16)
        spread = jnp.dot(pick, toks[span(which * rows, rows), :], preferred_element_type=jnp.float32)
        chosen = spread[:, 0:part]
        for q in range(1, CUTS):
            chosen = jnp.where(wcut == q, spread[:, q * part:(q + 1) * part], chosen)
        out_buf[span(g * gb, gb), :] = chosen.astype(jnp.bfloat16)
        each(g, target_of, lambda slot: give(slot).start())

    def real_group(g):
        return jnp.where(is_mid, (g + side) % groups, g)

    def near_send(i, c):
        g = near(i, 1)
        dispatch(g, 0, g)
        return c

    def far_send(i, c):
        g = far(i, 1)
        dispatch(g, guest, real_group(g))
        return c

    mine = span(me * block, block)
    theirs = span(partner * block, block)
    across = span(other * block, block)

    lax.fori_loop(0, side, near_send, 0)
    in_buf[mine, :] = out_buf[mine, :]

    for w in weights:
        w.wait()

    def send_back(g):
        each(g, carrier, lambda s: give_back(s).start())

    def experts(g):
        each(g, carrier, lambda s: take(s).wait_recv())
        here = span(g * gb, gb)
        stacked = jnp.dot(perm[...], in_buf[here, :], preferred_element_type=jnp.float32).astype(jnp.bfloat16)
        x = jnp.concatenate([stacked[q * gc:(q + 1) * gc, :] for q in range(CUTS)], axis=1)
        gate = jnp.dot(x, wg[...], preferred_element_type=jnp.float32)
        up = jnp.dot(x, wu[...], preferred_element_type=jnp.float32)
        hidden = (gate / (1.0 + jnp.exp(-gate)) * up).astype(jnp.bfloat16)
        y = jnp.dot(hidden, wd[...], preferred_element_type=jnp.float32).astype(jnp.bfloat16)
        back = jnp.concatenate([y[:, q * part:(q + 1) * part] for q in range(CUTS)], axis=0)
        wire = lax.dot_general(perm[...], back, (((0,), (0,)), ((), ())), preferred_element_type=jnp.float32)
        res_buf[here, :] = wire.astype(jnp.bfloat16)

    def far_experts(i, c):
        q = jnp.where(i < gq, 2 - half, 3 * (1 - half))
        g = q * gq + (mg + gq - i % gq) % gq
        experts(g)
        send_back(g)

        @pl.when(i == DEFER)
        def _():
            for k in range(PROMPT, side):
                send_back(near(k, -1))

        return c

    def near_then_swap(i, c):
        @pl.when(is_mid & (i == EARLY))
        def _():
            swaps[0].wait_recv()
            swaps[1].wait_recv()

        @pl.when(i == jnp.where(is_mid, EARLY, HELD))
        def _():
            lax.fori_loop(0, side, far_send, 0)

        @pl.when(is_mid & (i == EARLY))
        def _():
            in_buf[theirs, :] = out_buf[across, :]

        @pl.when(i < side)
        def _():
            experts(near(i, -1))

            @pl.when(i < PROMPT)
            def _():
                send_back(near(i, -1))

        return c

    lax.fori_loop(0, side + 1, near_then_swap, 0)
    lax.fori_loop(0, side, far_experts, 0)
    ret_buf[mine, :] = res_buf[mine, :]

    pcol = lax.broadcasted_iota(jnp.int32, (rows, gc), 1)

    def combine(first, which, shift):
        lines = meta[span(which * 8, 8), :]
        t0, t1, w0, w1 = columns([lines[i:i + 1, :] for i in range(4)])

        def step(i, c):
            g = first(i, 1)
            each(g, target_of, lambda slot: take_back(slot).wait_recv())
            stacked = jnp.dot(
                perm[...], ret_buf[span(g * gb, gb), :], preferred_element_type=jnp.float32
            ).astype(jnp.bfloat16)
            z = jnp.concatenate([stacked[q * gc:(q + 1) * gc, :] for q in range(CUTS)], axis=1)
            want = (pcol + shift(g) * gc).astype(jnp.float32)
            got0 = jnp.dot((t0 == want).astype(jnp.bfloat16), z, preferred_element_type=jnp.float32)
            got1 = jnp.dot((t1 == want).astype(jnp.bfloat16), z, preferred_element_type=jnp.float32)
            mixed[...] += got0 * w0 + got1 * w1
            return c

        lax.fori_loop(0, side, step, 0)

    mixed[...] = jnp.zeros_like(mixed)

    @pl.when(is_mid)
    def _():
        ret_buf[across, :] = res_buf[theirs, :]
        combine(far, guest, real_group)
        part_out[...] = mixed[...].astype(jnp.bfloat16)
        swaps[2].start()
        mixed[...] = jnp.zeros_like(mixed)

    combine(near, 0, lambda g: g)

    @pl.when(jnp.logical_not(is_mid))
    def _():
        combine(far, guest, real_group)

    @pl.when(is_mid)
    def _():
        swaps[2].wait_recv()
        mixed[...] += part_in[...].astype(jnp.float32)

    total = mixed[...]
    out_scale = lax.rsqrt(jnp.mean(total * total, axis=1, keepdims=True) + epsilon)
    out_ref[...] = (total * out_scale * post_ref[...]).astype(jnp.bfloat16)

    def drain(i, c):
        @pl.when(target_of(i) != me)
        def _():
            give(i).wait_send()

        @pl.when(carrier(i) != me)
        def _():
            give_back(i).wait_send()

        return c

    lax.fori_loop(0, n, drain, 0)

    @pl.when(is_mid)
    def _():
        for s in swaps:
            s.wait_send()


def fused(n, cap, tokens, pre_gain, post_gain, expert_ids, route_weights, w_gate, w_up, w_down):
    rows, width = tokens.shape
    hidden = w_gate.shape[2]
    part = width // CUTS
    block = CUTS * cap
    gb = GROUP * block
    vmem = pl.BlockSpec(memory_space=pltpu.VMEM)
    hbm = pl.BlockSpec(memory_space=pl.ANY)
    buf = pltpu.VMEM((n * block, part), jnp.bfloat16)
    return pl.pallas_call(
        functools.partial(fused_kernel, n, cap),
        out_shape=jax.ShapeDtypeStruct((rows, width), jnp.bfloat16),
        in_specs=[vmem] * 5 + [hbm] * 3,
        out_specs=vmem,
        scratch_shapes=[
            pltpu.VMEM((width, hidden), jnp.bfloat16),
            pltpu.VMEM((width, hidden), jnp.bfloat16),
            pltpu.VMEM((hidden, width), jnp.bfloat16),
            pltpu.VMEM((2 * rows, width), jnp.bfloat16),
            pltpu.VMEM((16, rows), jnp.float32),
            pltpu.VMEM((rows, width), jnp.bfloat16),
            pltpu.VMEM((rows, width), jnp.bfloat16),
            buf, buf, buf, buf,
            pltpu.VMEM((gb, gb), jnp.bfloat16),
            pltpu.VMEM((rows, width), jnp.float32),
            pltpu.SemaphoreType.DMA((3,)),
            pltpu.SemaphoreType.DMA((n,)),
            pltpu.SemaphoreType.DMA((n,)),
            pltpu.SemaphoreType.DMA((n,)),
            pltpu.SemaphoreType.DMA((n,)),
            pltpu.SemaphoreType.DMA((3,)),
            pltpu.SemaphoreType.DMA((3,)),
        ],
        compiler_params=pltpu.CompilerParams(collective_id=0, has_side_effects=True),
    )(
        tokens, pre_gain.reshape(1, width), post_gain.reshape(1, width), expert_ids.T, route_weights.T,
        w_gate, w_up, w_down,
    )


def per_device(tokens, pre_gain, post_gain, expert_ids, route_weights, w_gate, w_up, w_down):
    tok_rows, row_width = tokens.shape
    pick_count = expert_ids.shape[1]
    ep_count = lax.axis_size("ep")
    local_experts = w_gate.shape[0]
    experts = ep_count * local_experts
    capacity = 3 * tok_rows * pick_count // (2 * experts)
    pick_total = tok_rows * pick_count
    flat_ids = expert_ids.reshape(pick_total)
    onehot = (flat_ids[:, None] == jnp.arange(experts, dtype=jnp.int32)[None, :]).astype(
        jnp.bfloat16
    )
    positions = jnp.arange(pick_total, dtype=jnp.int32)
    strict_lower = (positions[None, :] < positions[:, None]).astype(jnp.bfloat16)
    earlier = jnp.dot(strict_lower, onehot, preferred_element_type=jnp.float32)
    slot_index = jnp.sum(earlier * onehot, axis=1).astype(jnp.int32)
    target = flat_ids * capacity + slot_index
    values = tokens.astype(jnp.float32)
    row_scale = lax.rsqrt(jnp.mean(values * values, axis=1, keepdims=True) + epsilon)
    normed = (values * row_scale * pre_gain[None, :]).astype(jnp.bfloat16)
    sent_width = normed.shape[1]
    copies = jnp.broadcast_to(normed[:, None, :], (tok_rows, pick_count, sent_width)).reshape(
        pick_total, sent_width
    )
    buffer = jnp.zeros((experts * capacity, sent_width), jnp.bfloat16).at[target].set(copies)
    arrived = lax.all_to_all(buffer, "ep", split_axis=0, concat_axis=0, tiled=True)
    rows_in = arrived.reshape(ep_count, local_experts, capacity, row_width)
    gate_sum = jnp.einsum("sxcd,xdf->sxcf", rows_in, w_gate, preferred_element_type=jnp.float32)
    up_sum = jnp.einsum("sxcd,xdf->sxcf", rows_in, w_up, preferred_element_type=jnp.float32)
    hidden = (jax.nn.silu(gate_sum) * up_sum).astype(jnp.bfloat16)
    out_cols = w_down.shape[2]
    produced = jnp.einsum(
        "sxcf,xfd->sxcd",
        lax.all_gather(hidden, "tp", axis=3, tiled=True),
        w_down,
        preferred_element_type=jnp.float32,
    )
    results = produced.astype(jnp.bfloat16).reshape(experts * capacity, out_cols)
    returned = lax.all_to_all(results, "ep", split_axis=0, concat_axis=0, tiled=True)
    picked = returned[target].astype(jnp.float32) * route_weights.reshape(pick_total)[:, None]
    mixed = jnp.sum(picked.reshape(tok_rows, pick_count, out_cols), axis=1)
    squares = lax.psum(jnp.sum(mixed * mixed, axis=1), "tp")
    out_scale = lax.rsqrt(squares / row_width + epsilon)
    return (mixed * out_scale[:, None] * post_gain[None, :]).astype(jnp.bfloat16)


def per_shard(n, tp, tokens, *rest):
    pre_gain, post_gain, expert_ids, route_weights, w_gate, w_up, w_down = rest
    rows, width = tokens.shape
    picks = expert_ids.shape[1]
    cap = 3 * rows * picks // (2 * n * w_gate.shape[0])
    fits = (
        tp == 1 and picks == 2 and w_gate.shape[0] == 1 and n % (4 * GROUP) == 0 and n <= 128
        and rows == 128 and (CUTS * cap) % 16 == 0 and cap > 0 and width % (CUTS * 128) == 0
    )
    if fits:
        return fused(n, cap, tokens, *rest)
    return per_device(tokens, *rest)


def solution(mesh):
    placed = (
        P("ep", None),
        P(),
        P("tp"),
        P("ep", None),
        P("ep", None),
        P("ep", None, "tp"),
        P("ep", None, "tp"),
        P("ep", None, "tp"),
    )
    return jax.shard_map(
        functools.partial(per_shard, mesh.shape["ep"], mesh.shape["tp"]),
        mesh=mesh, in_specs=placed, out_specs=P("ep", "tp"), check_vma=False,
    )
```

```python
import functools
import jax
import jax.numpy as jnp
from jax import lax
from jax.experimental import pallas as pl
from jax.experimental.pallas import tpu as pltpu
from jax.sharding import PartitionSpec as P

epsilon = 1e-06
CUTS = 4
GROUP = 4
EARLY = 2
GRANT = 60 * 1024 * 1024
HELD = 3
PROMPT = 0
DEFER = 3


def fused_kernel(
    n, cap, tok_ref, pre_ref, post_ref, ids_ref, rw_ref, wg_hbm, wu_hbm, wd_hbm, out_ref,
    wg, wu, wd, toks, meta, part_out, part_in, out_buf, in_buf, res_buf, ret_buf, perm, mixed,
    wsem, send1, recv1, send2, recv2, xsend, xrecv,
):
    rows, width = tok_ref.shape
    part = width // CUTS
    block = CUTS * cap
    gb = GROUP * block
    gc = GROUP * cap
    groups = n // GROUP
    side = groups // 2
    quarter = n // 4
    gq = groups // 4
    me = lax.axis_index("ep")
    tp = lax.axis_index("tp")
    mg = me // GROUP
    half = mg // side
    spot = mg % side
    plane = me // quarter
    is_mid = (plane == 1) | (plane == 2)
    partner = jnp.where(plane == 1, me + quarter, jnp.where(plane == 2, me - quarter, me))
    guest = jnp.where(is_mid, 1, 0)
    other = (me + n // 2) % n
    MESH = pl.DeviceIdType.MESH

    weights = [
        pltpu.make_async_copy(a.at[0], b, wsem.at[i])
        for i, (a, b) in enumerate(((wg_hbm, wg), (wu_hbm, wu), (wd_hbm, wd)))
    ]
    for w in weights:
        w.start()

    barrier = pltpu.get_barrier_semaphore()

    def greet(i, c):
        pl.semaphore_signal(barrier, inc=1, device_id=((me + i) % n, tp), device_id_type=MESH)
        return c

    lax.fori_loop(1, n, greet, 0)

    values = tok_ref[...].astype(jnp.float32)
    scale = lax.rsqrt(jnp.mean(values * values, axis=1, keepdims=True) + epsilon)
    toks[0:rows, :] = (values * scale * pre_ref[...]).astype(jnp.bfloat16)

    sub = lax.broadcasted_iota(jnp.int32, (rows, rows), 0)
    lane = lax.broadcasted_iota(jnp.int32, (rows, rows), 1)

    def columns(four):
        spread = jnp.where(sub == 3, four[3], 0.0)
        for i in range(3):
            spread = jnp.where(sub == i, four[i], spread)
        turned = spread.T
        return [turned[:, i:i + 1] for i in range(4)]

    w0row, w1row = rw_ref[0:1, :], rw_ref[1:2, :]
    ids0, ids1, _, _ = columns(
        [ids_ref[0:1, :].astype(jnp.float32), ids_ref[1:2, :].astype(jnp.float32), w0row, w1row]
    )
    expert = lane.astype(jnp.float32)
    hot0 = (ids0 == expert).astype(jnp.float32)
    hot1 = (ids1 == expert).astype(jnp.float32)
    tri = (lane < sub).astype(jnp.bfloat16)
    earlier = jnp.dot(tri, (hot0 + hot1).astype(jnp.bfloat16), preferred_element_type=jnp.float32)
    target0 = ids0 * cap + jnp.sum(earlier * hot0, axis=1, keepdims=True)
    target1 = ids1 * cap + jnp.sum(earlier * hot1, axis=1, keepdims=True)
    flipped = jnp.where(lane == 0, target0, jnp.where(lane == 1, target1, -1.0)).T
    eight = lax.broadcasted_iota(jnp.int32, (8, rows), 0)
    table = jnp.where(eight == 0, flipped[0:1, :], jnp.where(eight == 1, flipped[1:2, :], 0.0))
    meta[0:8, :] = jnp.where(eight == 2, w0row, jnp.where(eight == 3, w1row, table))

    def span(start, size):
        return pl.ds(pl.multiple_of(start, size), size)

    def swap(i, src, dst):
        return pltpu.make_async_remote_copy(
            src_ref=src, dst_ref=dst, send_sem=xsend.at[i], recv_sem=xrecv.at[i],
            device_id=(partner, tp), device_id_type=MESH,
        )

    swaps = [
        swap(0, meta.at[pl.ds(0, 8)], meta.at[pl.ds(8, 8)]),
        swap(1, toks.at[pl.ds(0, rows)], toks.at[pl.ds(rows, rows)]),
        swap(2, part_out, part_in),
    ]

    pl.semaphore_wait(barrier, n - 1)

    @pl.when(is_mid)
    def _():
        swaps[0].start()
        swaps[1].start()

    u = lax.broadcasted_iota(jnp.int32, (gb, gb), 0)
    v = lax.broadcasted_iota(jnp.int32, (gb, gb), 1)
    vu = (v % block) // cap * gc + v // block * cap + v % cap
    perm[...] = (u == vu).astype(jnp.bfloat16)

    wrow = lax.broadcasted_iota(jnp.int32, (gb, rows), 0)
    wslot = wrow // block * cap + wrow % cap
    wcut = (lax.broadcasted_iota(jnp.int32, (gb, part), 0) % block) // cap

    def relayed(slot):
        return is_mid & (slot // (n // 2) != half)

    def target_of(slot):
        return jnp.where(relayed(slot), (slot + n // 2) % n, slot)

    def guested(s):
        q = s // quarter
        return ((q == 1) | (q == 2)) & (s // (n // 2) != half)

    def carrier(s):
        q = s // quarter
        return jnp.where(guested(s), jnp.where(q == 1, s + quarter, s - quarter), s)

    def give(slot):
        source = jnp.where(relayed(slot), partner, me)
        return pltpu.make_async_remote_copy(
            src_ref=out_buf.at[span(slot * block, block)],
            dst_ref=in_buf.at[span(source * block, block)],
            send_sem=send1.at[slot], recv_sem=recv1.at[source],
            device_id=(target_of(slot), tp), device_id_type=MESH,
        )

    def take(s):
        return pltpu.make_async_remote_copy(
            src_ref=out_buf.at[span(s * block, block)],
            dst_ref=in_buf.at[span(s * block, block)],
            send_sem=send1.at[s], recv_sem=recv1.at[s],
            device_id=(carrier(s), tp), device_id_type=MESH,
        )

    def give_back(s):
        slot = jnp.where(guested(s), other, me)
        return pltpu.make_async_remote_copy(
            src_ref=res_buf.at[span(s * block, block)],
            dst_ref=ret_buf.at[span(slot * block, block)],
            send_sem=send2.at[s], recv_sem=recv2.at[slot],
            device_id=(carrier(s), tp), device_id_type=MESH,
        )

    def take_back(slot):
        return pltpu.make_async_remote_copy(
            src_ref=res_buf.at[span(slot * block, block)],
            dst_ref=ret_buf.at[span(slot * block, block)],
            send_sem=send2.at[slot], recv_sem=recv2.at[slot],
            device_id=(target_of(slot), tp), device_id_type=MESH,
        )

    def each(g, device, do):
        def one(j, c):
            index = g * GROUP + (me + j) % GROUP

            @pl.when(device(index) != me)
            def _():
                do(index)

            return c

        lax.fori_loop(0, GROUP, one, 0)

    def far(i, sign):
        return (1 - half) * side + (spot + side + sign * i) % side

    def near(i, sign):
        return half * side + (spot + side + sign * i) % side

    def dispatch(g, which, real):
        lines = meta[span(which * 8, 8), :]
        want = (wslot + real * gc).astype(jnp.float32)
        pick = ((lines[0:1, :] == want) | (lines[1:2, :] == want)).astype(jnp.bfloat16)
        spread = jnp.dot(pick, toks[span(which * rows, rows), :], preferred_element_type=jnp.float32)
        chosen = spread[:, 0:part]
        for q in range(1, CUTS):
            chosen = jnp.where(wcut == q, spread[:, q * part:(q + 1) * part], chosen)
        out_buf[span(g * gb, gb), :] = chosen.astype(jnp.bfloat16)
        each(g, target_of, lambda slot: give(slot).start())

    def real_group(g):
        return jnp.where(is_mid, (g + side) % groups, g)

    def near_send(i, c):
        g = near(i, 1)
        dispatch(g, 0, g)
        return c

    def far_send(i, c):
        g = far(i, 1)
        dispatch(g, guest, real_group(g))
        return c

    mine = span(me * block, block)
    theirs = span(partner * block, block)
    across = span(other * block, block)

    lax.fori_loop(0, side, near_send, 0)
    in_buf[mine, :] = out_buf[mine, :]

    for w in weights:
        w.wait()

    def send_back(g):
        each(g, carrier, lambda s: give_back(s).start())

    def experts(g):
        each(g, carrier, lambda s: take(s).wait_recv())
        here = span(g * gb, gb)
        stacked = jnp.dot(perm[...], in_buf[here, :], preferred_element_type=jnp.float32).astype(jnp.bfloat16)
        x = jnp.concatenate([stacked[q * gc:(q + 1) * gc, :] for q in range(CUTS)], axis=1)
        gate = jnp.dot(x, wg[...], preferred_element_type=jnp.float32)
        up = jnp.dot(x, wu[...], preferred_element_type=jnp.float32)
        hidden = (gate / (1.0 + jnp.exp(-gate)) * up).astype(jnp.bfloat16)
        y = jnp.dot(hidden, wd[...], preferred_element_type=jnp.float32).astype(jnp.bfloat16)
        back = jnp.concatenate([y[:, q * part:(q + 1) * part] for q in range(CUTS)], axis=0)
        wire = lax.dot_general(perm[...], back, (((0,), (0,)), ((), ())), preferred_element_type=jnp.float32)
        res_buf[here, :] = wire.astype(jnp.bfloat16)

    def far_experts(i, c):
        q = jnp.where(i < gq, 2 - half, 3 * (1 - half))
        g = q * gq + (mg + gq - i % gq) % gq
        experts(g)
        send_back(g)

        @pl.when(i == DEFER)
        def _():
            for k in range(PROMPT, side):
                send_back(near(k, -1))

        return c

    def near_then_swap(i, c):
        @pl.when(is_mid & (i == EARLY))
        def _():
            swaps[0].wait_recv()
            swaps[1].wait_recv()

        @pl.when(i == jnp.where(is_mid, EARLY, HELD))
        def _():
            lax.fori_loop(0, side, far_send, 0)

        @pl.when(is_mid & (i == EARLY))
        def _():
            in_buf[theirs, :] = out_buf[across, :]

        @pl.when(i < side)
        def _():
            experts(near(i, -1))

            @pl.when(i < PROMPT)
            def _():
                send_back(near(i, -1))

        return c

    lax.fori_loop(0, side + 1, near_then_swap, 0)
    lax.fori_loop(0, side, far_experts, 0)
    ret_buf[mine, :] = res_buf[mine, :]

    pcol = lax.broadcasted_iota(jnp.int32, (rows, gc), 1)

    def combine(first, which, shift):
        lines = meta[span(which * 8, 8), :]
        t0, t1, w0, w1 = columns([lines[i:i + 1, :] for i in range(4)])

        def step(i, c):
            g = first(i, 1)
            each(g, target_of, lambda slot: take_back(slot).wait_recv())
            stacked = jnp.dot(
                perm[...], ret_buf[span(g * gb, gb), :], preferred_element_type=jnp.float32
            ).astype(jnp.bfloat16)
            z = jnp.concatenate([stacked[q * gc:(q + 1) * gc, :] for q in range(CUTS)], axis=1)
            want = (pcol + shift(g) * gc).astype(jnp.float32)
            got0 = jnp.dot((t0 == want).astype(jnp.bfloat16), z, preferred_element_type=jnp.float32)
            got1 = jnp.dot((t1 == want).astype(jnp.bfloat16), z, preferred_element_type=jnp.float32)
            mixed[...] += got0 * w0 + got1 * w1
            return c

        lax.fori_loop(0, side, step, 0)

    mixed[...] = jnp.zeros_like(mixed)

    def given(i, c):
        @pl.when(target_of(i) != me)
        def _():
            give(i).wait_send()

        return c

    lax.fori_loop(0, n, given, 0)

    @pl.when(is_mid)
    def _():
        ret_buf[across, :] = res_buf[theirs, :]
        combine(far, guest, real_group)
        part_out[...] = mixed[...].astype(jnp.bfloat16)
        swaps[2].start()
        mixed[...] = jnp.zeros_like(mixed)

    combine(near, 0, lambda g: g)

    @pl.when(jnp.logical_not(is_mid))
    def _():
        combine(far, guest, real_group)

    @pl.when(is_mid)
    def _():
        swaps[2].wait_recv()
        mixed[...] += part_in[...].astype(jnp.float32)

    total = mixed[...]
    out_scale = lax.rsqrt(jnp.mean(total * total, axis=1, keepdims=True) + epsilon)
    out_ref[...] = (total * out_scale * post_ref[...]).astype(jnp.bfloat16)

    def drain(i, c):
        @pl.when(carrier(i) != me)
        def _():
            give_back(i).wait_send()

        return c

    lax.fori_loop(0, n, drain, 0)

    @pl.when(is_mid)
    def _():
        for s in swaps:
            s.wait_send()


def fused(n, cap, tokens, pre_gain, post_gain, expert_ids, route_weights, w_gate, w_up, w_down):
    rows, width = tokens.shape
    hidden = w_gate.shape[2]
    part = width // CUTS
    block = CUTS * cap
    gb = GROUP * block
    vmem = pl.BlockSpec(memory_space=pltpu.VMEM)
    hbm = pl.BlockSpec(memory_space=pltpu.HBM)
    buf = pltpu.VMEM((n * block, part), jnp.bfloat16)
    return pl.pallas_call(
        functools.partial(fused_kernel, n, cap),
        out_shape=jax.ShapeDtypeStruct((rows, width), jnp.bfloat16),
        in_specs=[vmem] * 5 + [hbm] * 3,
        out_specs=vmem,
        scratch_shapes=[
            pltpu.VMEM((width, hidden), jnp.bfloat16),
            pltpu.VMEM((width, hidden), jnp.bfloat16),
            pltpu.VMEM((hidden, width), jnp.bfloat16),
            pltpu.VMEM((2 * rows, width), jnp.bfloat16),
            pltpu.VMEM((16, rows), jnp.float32),
            pltpu.VMEM((rows, width), jnp.bfloat16),
            pltpu.VMEM((rows, width), jnp.bfloat16),
            buf, buf, buf, buf,
            pltpu.VMEM((gb, gb), jnp.bfloat16),
            pltpu.VMEM((rows, width), jnp.float32),
            pltpu.SemaphoreType.DMA((3,)),
            pltpu.SemaphoreType.DMA((n,)),
            pltpu.SemaphoreType.DMA((n,)),
            pltpu.SemaphoreType.DMA((n,)),
            pltpu.SemaphoreType.DMA((n,)),
            pltpu.SemaphoreType.DMA((3,)),
            pltpu.SemaphoreType.DMA((3,)),
        ],
        compiler_params=pltpu.CompilerParams(
            collective_id=0, has_side_effects=True, vmem_limit_bytes=GRANT
        ),
    )(
        tokens, pre_gain.reshape(1, width), post_gain.reshape(1, width), expert_ids.T, route_weights.T,
        w_gate, w_up, w_down,
    )


def per_device(tokens, pre_gain, post_gain, expert_ids, route_weights, w_gate, w_up, w_down):
    tok_rows, row_width = tokens.shape
    pick_count = expert_ids.shape[1]
    ep_count = lax.axis_size("ep")
    local_experts = w_gate.shape[0]
    experts = ep_count * local_experts
    capacity = 3 * tok_rows * pick_count // (2 * experts)
    pick_total = tok_rows * pick_count
    flat_ids = expert_ids.reshape(pick_total)
    onehot = (flat_ids[:, None] == jnp.arange(experts, dtype=jnp.int32)[None, :]).astype(
        jnp.bfloat16
    )
    positions = jnp.arange(pick_total, dtype=jnp.int32)
    strict_lower = (positions[None, :] < positions[:, None]).astype(jnp.bfloat16)
    earlier = jnp.dot(strict_lower, onehot, preferred_element_type=jnp.float32)
    slot_index = jnp.sum(earlier * onehot, axis=1).astype(jnp.int32)
    target = flat_ids * capacity + slot_index
    values = tokens.astype(jnp.float32)
    row_scale = lax.rsqrt(jnp.mean(values * values, axis=1, keepdims=True) + epsilon)
    normed = (values * row_scale * pre_gain[None, :]).astype(jnp.bfloat16)
    sent_width = normed.shape[1]
    copies = jnp.broadcast_to(normed[:, None, :], (tok_rows, pick_count, sent_width)).reshape(
        pick_total, sent_width
    )
    buffer = jnp.zeros((experts * capacity, sent_width), jnp.bfloat16).at[target].set(copies)
    arrived = lax.all_to_all(buffer, "ep", split_axis=0, concat_axis=0, tiled=True)
    rows_in = arrived.reshape(ep_count, local_experts, capacity, row_width)
    gate_sum = jnp.einsum("sxcd,xdf->sxcf", rows_in, w_gate, preferred_element_type=jnp.float32)
    up_sum = jnp.einsum("sxcd,xdf->sxcf", rows_in, w_up, preferred_element_type=jnp.float32)
    hidden = (jax.nn.silu(gate_sum) * up_sum).astype(jnp.bfloat16)
    out_cols = w_down.shape[2]
    produced = jnp.einsum(
        "sxcf,xfd->sxcd",
        lax.all_gather(hidden, "tp", axis=3, tiled=True),
        w_down,
        preferred_element_type=jnp.float32,
    )
    results = produced.astype(jnp.bfloat16).reshape(experts * capacity, out_cols)
    returned = lax.all_to_all(results, "ep", split_axis=0, concat_axis=0, tiled=True)
    picked = returned[target].astype(jnp.float32) * route_weights.reshape(pick_total)[:, None]
    mixed = jnp.sum(picked.reshape(tok_rows, pick_count, out_cols), axis=1)
    squares = lax.psum(jnp.sum(mixed * mixed, axis=1), "tp")
    out_scale = lax.rsqrt(squares / row_width + epsilon)
    return (mixed * out_scale[:, None] * post_gain[None, :]).astype(jnp.bfloat16)


def per_shard(n, tp, tokens, *rest):
    pre_gain, post_gain, expert_ids, route_weights, w_gate, w_up, w_down = rest
    rows, width = tokens.shape
    picks = expert_ids.shape[1]
    cap = 3 * rows * picks // (2 * n * w_gate.shape[0])
    fits = (
        tp == 1 and picks == 2 and w_gate.shape[0] == 1 and n % (4 * GROUP) == 0 and n <= 128
        and rows == 128 and (CUTS * cap) % 16 == 0 and cap > 0 and width % (CUTS * 128) == 0
    )
    if fits:
        return fused(n, cap, tokens, *rest)
    return per_device(tokens, *rest)


def solution(mesh):
    placed = (
        P("ep", None),
        P(),
        P("tp"),
        P("ep", None),
        P("ep", None),
        P("ep", None, "tp"),
        P("ep", None, "tp"),
        P("ep", None, "tp"),
    )
    return jax.shard_map(
        functools.partial(per_shard, mesh.shape["ep"], mesh.shape["tp"]),
        mesh=mesh, in_specs=placed, out_specs=P("ep", "tp"), check_vma=False,
    )
```
